512 devices in a mesh: kv: 16 (over y, x), tp: 32 (over z, core).
Axes of the slice: x: 4, y: 4, z: 16, core: 2. Of those that a mesh axis runs over, the one named last changes fastest.
Arguments:
- tokens: bfloat16 [128, 4096], P(None, ('kv', 'tp')), may hold values from -60 to 60, as said below
- gain_mix: float32 [4096], replicated, may hold values from 0.1 to 1.9
- w_query: bfloat16 [4096, 4096], P('kv', 'tp'), may hold values from -0.09375 to 0.09375
- w_key: bfloat16 [4096, 4096], P('kv', 'tp'), may hold values from -0.75 to 0.75
- w_value: bfloat16 [4096, 4096], P('kv', 'tp'), may hold values from -0.09375 to 0.09375
- w_outgate: bfloat16 [4096, 4096], P('kv', 'tp'), may hold values from -0.09375 to 0.09375
- w_gates: bfloat16 [4096, 32], P('kv'), may hold values from -0.09375 to 0.09375
- forget_bias: float32 [16], replicated, may hold values from 0 to 4
- cell_state: float32 [128, 4096, 256], P('kv', 'tp'), may hold values from -1.5 to 1.5
- norm_state: float32 [128, 16, 256], P('kv'), may hold values from -1.5 to 1.5
- max_state: float32 [128, 16], P('kv'), may hold values from -1 to 2
- gain_group: float32 [4096], replicated, may hold values from 0.1 to 1.9
- w_mix: bfloat16 [4096, 4096], P('tp', 'kv'), may hold values from -0.1875 to 0.1875
- gain_ffn: float32 [4096], replicated, may hold values from 0.1 to 1.9
- w_up: bfloat16 [4096, 16384], P('kv', 'tp'), may hold values from -0.09375 to 0.09375
- w_down: bfloat16 [16384, 4096], P('tp', 'kv'), may hold values from -0.09375 to 0.09375
Outputs:
- layer_out: bfloat16 [128, 4096], P(None, ('kv', 'tp'))
- cell_next: float32 [128, 4096, 256], P('kv', 'tp')
- norm_next: float32 [128, 16, 256], P('kv')
- max_next: float32 [128, 16], P('kv')
The draws below stay inside these ranges and needn't reach their ends.
Inputs may be any that keep to these rules, and one draw needn't show every extreme that they name: `tokens`: finite activations.
All inputs are finite; a program needn't handle non-finite values.
Results may differ from the reference program's by a relative error of at most 0.019.
Values may be sent and summed in bfloat16 or wider, within the bound.
A program may use at most 64 MiB of HBM per device.

```python
import math
import jax
import jax.numpy as jnp
from jax import lax

D = 4096
HEADS = 16
HEAD_DIM = 256
FF = 16384
BATCH = 128


def draw_tokens(key, part):
    first = jax.random.fold_in(jax.random.fold_in(key, 11), 0)
    columns = jnp.arange(D, dtype=jnp.float32) / D
    base = jnp.clip(jax.random.normal(first, (BATCH, D), jnp.float32), -6.0, 6.0)
    col_scale = 0.3 * jnp.exp(columns * math.log(10.0))
    values = base * col_scale
    return values.astype(jnp.bfloat16)


def with_spikes(result, stream_key, source, target, blocks, factor):
    owner, partner = [(jnp.arange(result.shape[axis_at]) // (result.shape[axis_at] // blocks)).reshape([-1 if axis == axis_at else 1 for axis in range(result.ndim)]) for axis_at in (source, target)]
    chosen = jax.random.permutation(stream_key, blocks)[partner]
    strong = (owner == chosen) | (owner == (partner + blocks // 2) % blocks)
    return jnp.where(strong, factor * result, result)


def level_of(own_key, extent, shards, least, top_value):
    def one(position, parts):
        draws = jax.random.uniform(jax.random.fold_in(jax.random.fold_in(own_key, 6), position), (parts,), jnp.float32, least / len(shards), top_value / len(shards))
        return jnp.repeat(jnp.exp(draws), extent[position] // parts).reshape((-1,) + (1,) * (len(extent) - position - 1))

    gain = one(*shards[0])
    for cut in shards[1:]:
        gain = gain * one(*cut)
    return gain


def bell_draw(own_key, shape, scale, bound, cuts=(), kind=jnp.bfloat16):
    entries = jax.random.normal(own_key, shape, jnp.float32) * scale
    if len(cuts) > 0:
        entries = level_of(own_key, shape, cuts, -0.22, 0.18) * entries
    return jnp.clip(entries, min=-bound, max=bound).astype(kind)


def bell_draw_with(stream_key, extent, scale, bound, cuts, heavy, kind=jnp.bfloat16):
    array = scale * jax.random.normal(stream_key, extent, jnp.float32)
    if cuts:
        array = array * level_of(stream_key, extent, cuts, -0.22, 0.18)
    return jnp.clip(with_spikes(array, jax.random.fold_in(stream_key, 3), *heavy), -bound, bound).astype(kind)


def setup_inputs(seed: int = 0) -> dict:
    key_list = jax.random.split(jax.random.key(seed), 17)
    return {
        "tokens": draw_tokens(jax.random.fold_in(key_list[16], 71), 0),
        "gain_mix": jnp.clip(1.0 + 0.18 * jax.random.normal(key_list[1], (D,), jnp.float32), 0.1, 1.9),
        "w_query": bell_draw(key_list[2], (D, HEADS * HEAD_DIM), D ** -0.5, 0.09375, ((0, 16), (1, 32))),
        "w_key": bell_draw(key_list[3], (D, HEADS * HEAD_DIM), (D // 64) ** -0.5, 0.75, ((0, 16), (1, 32))),
        "w_value": bell_draw(key_list[4], (D, HEADS * HEAD_DIM), D ** -0.5, 0.09375, ((0, 16), (1, 32))),
        "w_outgate": bell_draw(key_list[5], (D, HEADS * HEAD_DIM), D ** -0.5, 0.09375, ((0, 16), (1, 32))),
        "w_gates": bell_draw(key_list[6], (D, 2 * HEADS), D ** -0.5, 0.09375, ((0, 16),)),
        "forget_bias": jnp.clip(jax.random.uniform(key_list[7], (HEADS,), jnp.float32, 0.0, 4.0), 0.0, 4.0),
        "cell_state": bell_draw(key_list[8], (BATCH, HEADS * HEAD_DIM, HEAD_DIM), 0.25, 1.5, ((0, 16), (1, 32)), jnp.float32),
        "norm_state": bell_draw(key_list[9], (BATCH, HEADS, HEAD_DIM), 0.25, 1.5, ((0, 16),), jnp.float32),
        "max_state": jnp.clip(-1.0 + 3.0 * jax.random.uniform(key_list[10], (BATCH, HEADS), jnp.float32) ** level_of(key_list[10], (BATCH, HEADS), ((0, 16),), -0.2, 0.2), -1.0, 2.0),
        "gain_group": jnp.clip(1.0 + 0.18 * jax.random.normal(key_list[11], (HEADS * HEAD_DIM,), jnp.float32), 0.1, 1.9),
        "w_mix": bell_draw_with(key_list[12], (HEADS * HEAD_DIM, D), (HEADS * HEAD_DIM) ** -0.5, 0.1875, ((0, 32), (1, 16)), (0, 1, 32, 2.75)),
        "gain_ffn": jnp.clip(1.0 + 0.18 * jax.random.normal(key_list[13], (D,), jnp.float32), 0.1, 1.9),
        "w_up": bell_draw(key_list[14], (D, FF), D ** -0.5, 0.09375, ((0, 16), (1, 32))),
        "w_down": bell_draw_with(key_list[15], (FF, D), FF ** -0.5, 0.09375, ((0, 32), (1, 16)), (0, 1, 32, 2.75)),
    }


EPSILON = 1e-06

def reference(tokens, gain_mix, w_query, w_key, w_value, w_outgate, w_gates, forget_bias, cell_state, norm_state, max_state, gain_group, w_mix, gain_ffn, w_up, w_down):
    f32 = jnp.float32
    bf16 = jnp.bfloat16
    batch = tokens.shape[0]
    xf = tokens.astype(f32)
    scale_in = lax.rsqrt(lax.optimization_barrier(jnp.mean(xf * xf, axis=1, keepdims=True)) + EPSILON)
    normed = (xf * gain_mix).astype(bf16)
    query = (jnp.dot(normed, w_query, preferred_element_type=f32) * scale_in).astype(bf16)
    keys = (jnp.dot(normed, w_key, preferred_element_type=f32) * scale_in).astype(bf16)
    values = jnp.dot(normed, w_value, preferred_element_type=f32) * scale_in
    gate_out = jnp.dot(normed, w_outgate, preferred_element_type=f32) * scale_in
    gates = jnp.dot(normed, w_gates, preferred_element_type=f32) * scale_in
    gate_in = gates[:, :HEADS]
    log_forget = jax.nn.log_sigmoid(gates[:, HEADS:] + forget_bias)
    max_next = jnp.maximum(log_forget + max_state, gate_in)
    decay = jnp.exp(log_forget + max_state - max_next)
    inflow = jnp.exp(gate_in - max_next)
    qf = query.astype(f32).reshape(batch, HEADS, HEAD_DIM)
    kf = keys.astype(f32).reshape(batch, HEADS, HEAD_DIM) / math.sqrt(HEAD_DIM)
    vh = values.reshape(batch, HEADS, HEAD_DIM)
    cells = cell_state.reshape(batch, HEADS, HEAD_DIM, HEAD_DIM)
    cell_next = decay[..., None, None] * cells + inflow[..., None, None] * vh[..., :, None] * kf[..., None, :]
    norm_next = decay[..., None] * norm_state + inflow[..., None] * kf
    numer = jnp.einsum('bhvk,bhk->bhv', cell_next, qf, precision=lax.Precision.HIGHEST)
    denom = jnp.maximum(jnp.abs(lax.optimization_barrier(jnp.sum(norm_next * qf, axis=-1))), 1.0)
    cell_read = (jax.nn.sigmoid(gate_out) * (numer / denom[..., None]).reshape(batch, HEADS * HEAD_DIM)).astype(bf16)
    readf = cell_read.astype(f32)
    scale_group = lax.rsqrt(lax.optimization_barrier(jnp.mean(readf * readf, axis=1, keepdims=True)) + EPSILON)
    grouped = (readf * gain_group).astype(bf16)
    mixed = (xf + jnp.dot(grouped, w_mix, preferred_element_type=f32) * scale_group).astype(bf16)
    mixf = mixed.astype(f32)
    scale_ffn = lax.rsqrt(lax.optimization_barrier(jnp.mean(mixf * mixf, axis=1, keepdims=True)) + EPSILON)
    normed_ffn = (mixf * gain_ffn).astype(bf16)
    hidden = jnp.square(jax.nn.relu(jnp.dot(normed_ffn, w_up, preferred_element_type=f32) * scale_ffn)).astype(bf16)
    layer_out = (mixf + jnp.dot(hidden, w_down, preferred_element_type=f32)).astype(bf16)
    return (layer_out, cell_next.reshape(batch, HEADS * HEAD_DIM, HEAD_DIM), norm_next, max_next)
```

```python
import functools
import math

import jax
import jax.numpy as jnp
from jax import lax
from jax.experimental import pallas as pl
from jax.experimental.pallas import tpu as pltpu
from jax.sharding import PartitionSpec as P

EPSILON = 1e-06
F32 = jnp.float32
BF16 = jnp.bfloat16
MESH = pl.DeviceIdType.MESH


def dot(a, b, ca, cb):
    return lax.dot_general(a, b, (((ca,), (cb,)), ((), ())), preferred_element_type=F32)


def kernel(
    nkv,
    ntp,
    width,
    tok_ref,
    gmix_ref,
    wq_ref,
    wk_ref,
    wv_ref,
    wo_ref,
    wgt_ref,
    bias_ref,
    cell_ref,
    norm_ref,
    max_ref,
    ggrp_ref,
    wmix_ref,
    gffn_ref,
    wup_ref,
    wdown_ref,
    out_ref,
    cellnext_ref,
    normnext_ref,
    maxnext_ref,
    tok,
    gmix,
    w4,
    wgt,
    bias,
    cell,
    norm,
    maxs,
    ggrp,
    wmix,
    gffn,
    wup,
    wdown,
    wbig,
    wmixt,
    wupt,
    wdownt,
    cellb,
    ones_tail,
    a_recv,
    b_send,
    b_recv,
    p_send,
    p_recv,
    k_recv,
    c_send,
    c_recv,
    d_send,
    d_recv,
    dsq_send,
    dsq_recv,
    e_send,
    e_recv,
    f_send,
    f_recv,
    fsq_send,
    fsq_recv,
    g_send,
    g_recv,
    h_send,
    h_recv,
    load_sems,
    send_sems,
    recv_sems,
    out_sems,
):
    kv = lax.axis_index("kv")
    tp = lax.axis_index("tp")
    seqs, rows, hd = cell.shape
    heads = norm.shape[1]
    cols, batch = tok.shape
    block = cols * ntp
    share = f_send.shape[1]
    units = share * nkv
    head = tp * rows // hd
    side = tp % 2

    barrier = pltpu.get_barrier_semaphore()

    def greet_tp(i, _):
        pl.semaphore_signal(
            barrier, inc=1, device_id=(kv, lax.rem(tp + i, ntp)), device_id_type=MESH
        )
        return 0

    def greet_kv(i, _):
        pl.semaphore_signal(
            barrier, inc=1, device_id=(lax.rem(kv + i, nkv), tp), device_id_type=MESH
        )
        return 0

    lax.fori_loop(1, ntp, greet_tp, 0)
    lax.fori_loop(1, nkv, greet_kv, 0)

    loads = []
    for i, (src, dst) in enumerate(
        (
            (tok_ref, tok),
            (gmix_ref, gmix),
            (wq_ref, w4.at[0]),
            (wk_ref, w4.at[1]),
            (wv_ref, w4.at[2]),
            (wo_ref, w4.at[3]),
            (wgt_ref, wgt),
            (bias_ref, bias),
            (cell_ref, cell),
            (norm_ref, norm),
            (max_ref, maxs),
            (ggrp_ref, ggrp),
            (wmix_ref, wmix),
            (gffn_ref, gffn),
            (wup_ref, wup),
            (wdown_ref, wdown),
        )
    ):
        copy = pltpu.make_async_copy(src, dst, load_sems.at[i])
        copy.start()
        loads.append(copy)

    def tp_peer(i):
        half = ntp // 2
        return lax.rem(tp + half + (1 - 2 * (i % 2)) * ((i + 1) // 2) + ntp, ntp)

    def kv_peer(i):
        half = nkv // 2
        return lax.rem(kv + half + (1 - 2 * (i % 2)) * ((i + 1) // 2) + nkv, nkv)

    def push(phase, src, dst, device):
        pltpu.make_async_remote_copy(
            src_ref=src,
            dst_ref=dst,
            send_sem=send_sems.at[phase],
            recv_sem=recv_sems.at[phase],
            device_id=device,
            device_id_type=MESH,
        ).start()

    def send_tp(phase, src_of, dst):
        def one(i, _):
            peer = tp_peer(i)
            push(phase, src_of(peer), dst.at[tp], (kv, peer))
            return 0

        lax.fori_loop(0, ntp - 1, one, 0)

    def send_kv(phase, src_of, dst):
        def one(i, _):
            peer = kv_peer(i)
            push(phase, src_of(peer), dst.at[kv], (peer, tp))
            return 0

        lax.fori_loop(0, nkv - 1, one, 0)

    def all_of(phase, buf, count):
        part = buf.at[pl.ds(0, count)]
        return pltpu.make_async_remote_copy(
            src_ref=part,
            dst_ref=part,
            send_sem=send_sems.at[phase],
            recv_sem=recv_sems.at[phase],
            device_id=(kv, lax.rem(tp + 1, ntp)),
            device_id_type=MESH,
        )

    loads[0].wait()
    pl.semaphore_wait(barrier, ntp - 1 + nkv - 1)
    send_tp(0, lambda peer: tok, a_recv)
    a_recv[tp] = tok[...]

    for i in range(1, 16):
        loads[i].wait()
    lane_groups = block // 128 if block >= 128 else 1
    lanes = block // lane_groups
    gpieces = []
    for g in range(lane_groups):
        row = gmix[pl.ds(kv * lane_groups + g, 1), :]
        gpieces.append(jnp.transpose(jnp.broadcast_to(row, (128, lanes))))
    gain_col = jnp.concatenate(gpieces, axis=0)
    for i in range(4):
        wbig[:, i * rows : (i + 1) * rows] = (
            w4[i].astype(F32) * gain_col[:, :rows]
        ).astype(BF16)
    wg = jnp.transpose(wgt[...].astype(F32)) * gain_col[:, : 2 * heads]
    wbig[:, 4 * rows :] = jnp.zeros((block, 128), BF16)
    wbig[:, 4 * rows : 4 * rows + 2 * heads] = wg.astype(BF16)
    lane_id = lax.broadcasted_iota(jnp.int32, (block, 128), 1)
    ones_tail[...] = jnp.where(lane_id < 2 * heads, 0.0, 1.0).astype(BF16)
    grow = ggrp[pl.ds(tp, 1), :]
    wmixt[...] = (jnp.transpose(wmix[...].astype(F32)) * grow).astype(BF16)
    frow = jnp.concatenate(
        [gffn[pl.ds(kv * lane_groups + g, 1), :] for g in range(lane_groups)], axis=1
    )
    wupt[...] = (jnp.transpose(wup[...].astype(F32)) * frow).astype(BF16)
    wdownt[...] = jnp.transpose(wdown[...].astype(F32)).astype(BF16)
    for s in range(seqs):
        cellb[s] = cell[s].astype(BF16)
    head_of = lax.broadcasted_iota(jnp.int32, (seqs, heads, hd), 1)
    norm_own = jnp.sum(jnp.where(head_of == head, norm[...], 0.0), axis=1)

    all_of(0, a_recv, ntp - 1).wait_recv()
    xf = a_recv[...].astype(F32).reshape(block, batch)
    xb = xf.astype(BF16)
    xsq = (xf * xf).astype(BF16)
    part = dot(xb, wbig[...], 0, 0)
    tail = dot(xsq, ones_tail[...], 0, 0)
    b_send[:, :, : 4 * rows] = part[:, : 4 * rows].reshape(nkv, seqs, 4 * rows).astype(BF16)
    b_send[:, :, 4 * rows :] = (
        (part[:, 4 * rows :] + tail).reshape(nkv, seqs, 128).astype(BF16)
    )
    send_kv(1, lambda peer: b_send.at[peer], b_recv)
    b_recv[kv] = b_send[kv]
    all_of(1, b_recv, nkv - 1).wait_recv()
    total = b_recv[0].astype(F32)
    for j in range(1, nkv):
        total = total + b_recv[j].astype(F32)
    scale_in = lax.rsqrt(
        total[:, 4 * rows + 2 * heads : 4 * rows + 2 * heads + 1] / width + EPSILON
    )
    total = total * scale_in
    q_part = total[:, :rows].astype(BF16)
    k_part = total[:, rows : 2 * rows].astype(BF16)
    values = total[:, 2 * rows : 3 * rows]
    gate_out = total[:, 3 * rows : 4 * rows]
    gate_in = total[:, 4 * rows : 4 * rows + heads]
    gate_forget = total[:, 4 * rows + heads : 4 * rows + 2 * heads]

    p_send[0] = q_part
    p_send[1] = k_part
    sibling = tp + 1 - 2 * side
    pair = pltpu.make_async_remote_copy(
        src_ref=p_send,
        dst_ref=p_recv,
        send_sem=send_sems.at[2],
        recv_sem=recv_sems.at[2],
        device_id=(kv, sibling),
        device_id_type=MESH,
    )
    pair.start()

    arg = gate_forget + bias[...]
    log_forget = jnp.minimum(arg, 0.0) - jnp.log1p(jnp.exp(-jnp.abs(arg)))
    carried = log_forget + maxs[...]
    max_next = jnp.maximum(carried, gate_in)
    decay = jnp.exp(carried - max_next)
    inflow = jnp.exp(gate_in - max_next)
    maxnext_ref[...] = max_next
    head_lane = lax.broadcasted_iota(jnp.int32, (seqs, heads), 1)
    dec = jnp.sum(jnp.where(head_lane == head, decay, 0.0), axis=1, keepdims=True)
    inf = jnp.sum(jnp.where(head_lane == head, inflow, 0.0), axis=1, keepdims=True)
    gate_sig = jax.nn.sigmoid(gate_out)

    pair.wait_recv()
    q_other = p_recv[0].astype(F32)
    k_other = p_recv[1].astype(F32)
    q_mine = q_part.astype(F32)
    k_mine = k_part.astype(F32)
    first = side == 0
    qf = jnp.concatenate(
        [jnp.where(first, q_mine, q_other), jnp.where(first, q_other, q_mine)], axis=1
    )
    kf = jnp.concatenate(
        [jnp.where(first, k_mine, k_other), jnp.where(first, k_other, k_mine)], axis=1
    ) / math.sqrt(hd)
    kq = jnp.sum(kf * qf, axis=1, keepdims=True)
    nq = jnp.sum(norm_own * qf, axis=1, keepdims=True)
    denom = jnp.maximum(jnp.abs(dec * nq + inf * kq), 1.0)
    row_id = lax.broadcasted_iota(jnp.int32, (seqs, hd), 0)
    cq = jnp.zeros((seqs, rows), F32)
    for s in range(seqs):
        cq = cq + dot(jnp.where(row_id == s, qf, 0.0).astype(BF16), cellb[s], 1, 1)
    iv = inf * values
    read = gate_sig * ((dec * cq + iv * kq) / denom)

    c_send[...] = read.astype(BF16)
    send_kv(3, lambda peer: c_send, c_recv)
    c_recv[kv] = c_send[...]
    send_tp(4, lambda peer: p_send.at[1], k_recv)
    k_recv[tp] = p_send[1]
    ivt = jnp.transpose(iv)
    for s in range(seqs):
        cell[s] = dec[s : s + 1, :] * cell[s] + ivt[:, s : s + 1] * kf[s : s + 1, :]
    cell_out = pltpu.make_async_copy(cell, cellnext_ref, out_sems.at[0])
    cell_out.start()

    all_of(3, c_recv, nkv - 1).wait_recv()
    rf = c_recv[...].astype(F32).reshape(batch, rows)
    rb = rf.astype(BF16)
    sq = dot(jnp.ones((8, rows), BF16), (rf * rf).astype(BF16), 1, 1)
    dsq_send[...] = sq[0:1, :]
    mixt = dot(wmixt[...], rb, 1, 1)
    d_send[...] = mixt.reshape(ntp, cols, batch).astype(BF16)
    send_tp(5, lambda peer: d_send.at[peer], d_recv)
    send_tp(6, lambda peer: dsq_send, dsq_recv)
    d_recv[tp] = d_send[tp]
    dsq_recv[tp] = dsq_send[...]
    all_of(5, d_recv, ntp - 1).wait_recv()
    all_of(6, dsq_recv, ntp - 1).wait_recv()
    mix_sum = d_recv[0].astype(F32)
    sq_sum = dsq_recv[0]
    for j in range(1, ntp):
        mix_sum = mix_sum + d_recv[j].astype(F32)
        sq_sum = sq_sum + dsq_recv[j]
    scale_group = lax.rsqrt(sq_sum / (heads * hd) + EPSILON)
    mixed = (tok[...].astype(F32) + mix_sum * scale_group).astype(BF16)

    e_send[...] = mixed
    send_tp(7, lambda peer: e_send, e_recv)
    e_recv[tp] = e_send[...]
    all_of(7, e_recv, ntp - 1).wait_recv()
    mf = e_recv[...].astype(F32).reshape(block, batch)
    fsq_send[...] = jnp.sum(mf * mf, axis=0, keepdims=True)
    send_kv(8, lambda peer: fsq_send, fsq_recv)
    fsq_recv[kv] = fsq_send[...]
    upt = dot(wupt[...], mf.astype(BF16), 1, 0)
    f_send[...] = upt.reshape(nkv, share, batch).astype(BF16)
    send_kv(9, lambda peer: f_send.at[peer], f_recv)
    f_recv[kv] = f_send[kv]
    all_of(8, fsq_recv, nkv - 1).wait_recv()
    fsq_sum = fsq_recv[0]
    for j in range(1, nkv):
        fsq_sum = fsq_sum + fsq_recv[j]
    scale_ffn = lax.rsqrt(fsq_sum / width + EPSILON)
    all_of(9, f_recv, nkv - 1).wait_recv()
    up = f_recv[0].astype(F32)
    for j in range(1, nkv):
        up = up + f_recv[j].astype(F32)
    hid = jnp.maximum(up * scale_ffn, 0.0)

    g_send[...] = (hid * hid).astype(BF16)
    send_kv(10, lambda peer: g_send, g_recv)
    g_recv[kv] = g_send[...]
    all_of(4, k_recv, ntp - 1).wait_recv()
    per_head = hd // rows
    for h in range(heads):
        key = jnp.concatenate(
            [k_recv[h * per_head + i].astype(F32) for i in range(per_head)], axis=1
        ) / math.sqrt(hd)
        norm[:, h, :] = decay[:, h : h + 1] * norm[:, h, :] + inflow[:, h : h + 1] * key
    norm_out = pltpu.make_async_copy(norm, normnext_ref, out_sems.at[1])
    norm_out.start()

    all_of(10, g_recv, nkv - 1).wait_recv()
    hidden = g_recv[...].reshape(units, batch)
    downt = dot(wdownt[...], hidden, 1, 0)
    h_send[...] = downt.reshape(ntp, cols, batch).astype(BF16)
    send_tp(11, lambda peer: h_send.at[peer], h_recv)
    h_recv[tp] = h_send[tp]

    all_of(0, a_recv, ntp - 1).wait_send()
    all_of(1, b_recv, nkv - 1).wait_send()
    pair.wait_send()
    all_of(3, c_recv, nkv - 1).wait_send()
    all_of(4, k_recv, ntp - 1).wait_send()
    all_of(5, d_recv, ntp - 1).wait_send()
    all_of(6, dsq_recv, ntp - 1).wait_send()
    all_of(7, e_recv, ntp - 1).wait_send()
    all_of(8, fsq_recv, nkv - 1).wait_send()
    all_of(9, f_recv, nkv - 1).wait_send()
    all_of(10, g_recv, nkv - 1).wait_send()
    cell_out.wait()
    norm_out.wait()

    all_of(11, h_recv, ntp - 1).wait_recv()
    down = h_recv[0].astype(F32)
    for j in range(1, ntp):
        down = down + h_recv[j].astype(F32)
    out_ref[...] = (mixed.astype(F32) + down).astype(BF16)
    all_of(11, h_recv, ntp - 1).wait_send()


def per_device(nkv, ntp, *args):
    (
        tokens,
        gain_mix,
        w_query,
        w_key,
        w_value,
        w_outgate,
        w_gates,
        forget_bias,
        cell_state,
        norm_state,
        max_state,
        gain_group,
        w_mix,
        gain_ffn,
        w_up,
        w_down,
    ) = args
    batch, cols = tokens.shape
    width = gain_mix.shape[0]
    seqs, rows, hd = cell_state.shape
    heads = forget_bias.shape[0]
    block = w_query.shape[0]
    units = w_up.shape[1]
    share = units // nkv
    lanes = min(block, 128)
    operands = (
        tokens.T,
        gain_mix.reshape(-1, lanes),
        w_query,
        w_key,
        w_value,
        w_outgate,
        w_gates.T,
        forget_bias.reshape(1, heads),
        cell_state,
        norm_state,
        max_state,
        gain_group.reshape(-1, rows),
        w_mix,
        gain_ffn.reshape(-1, lanes),
        w_up,
        w_down,
    )
    wide = 4 * rows + 128
    vmem = pltpu.VMEM
    scratch = [
        vmem((cols, batch), BF16),
        vmem((width // lanes, lanes), F32),
        vmem((4, block, rows), BF16),
        vmem((2 * heads, block), BF16),
        vmem((1, heads), F32),
        vmem((seqs, rows, hd), F32),
        vmem((seqs, heads, hd), F32),
        vmem((seqs, heads), F32),
        vmem((heads * hd // rows, rows), F32),
        vmem((rows, block), BF16),
        vmem((width // lanes, lanes), F32),
        vmem((block, units), BF16),
        vmem((units, block), BF16),
        vmem((block, wide), BF16),
        vmem((block, rows), BF16),
        vmem((units, block), BF16),
        vmem((block, units), BF16),
        vmem((seqs, rows, hd), BF16),
        vmem((block, 128), BF16),
        vmem((ntp, cols, batch), BF16),
        vmem((nkv, seqs, wide), BF16),
        vmem((nkv, seqs, wide), BF16),
        vmem((2, seqs, rows), BF16),
        vmem((2, seqs, rows), BF16),
        vmem((ntp, seqs, rows), BF16),
        vmem((seqs, rows), BF16),
        vmem((nkv, seqs, rows), BF16),
        vmem((ntp, cols, batch), BF16),
        vmem((ntp, cols, batch), BF16),
        vmem((1, batch), F32),
        vmem((ntp, 1, batch), F32),
        vmem((cols, batch), BF16),
        vmem((ntp, cols, batch), BF16),
        vmem((nkv, share, batch), BF16),
        vmem((nkv, share, batch), BF16),
        vmem((1, batch), F32),
        vmem((nkv, 1, batch), F32),
        vmem((share, batch), BF16),
        vmem((nkv, share, batch), BF16),
        vmem((ntp, cols, batch), BF16),
        vmem((ntp, cols, batch), BF16),
        pltpu.SemaphoreType.DMA((16,)),
        pltpu.SemaphoreType.DMA((12,)),
        pltpu.SemaphoreType.DMA((12,)),
        pltpu.SemaphoreType.DMA((2,)),
    ]
    anywhere = pl.BlockSpec(memory_space=pl.ANY)
    in_vmem = pl.BlockSpec(memory_space=pltpu.VMEM)
    out, cell_next, norm_next, max_next = pl.pallas_call(
        functools.partial(kernel, nkv, ntp, width),
        out_shape=(
            jax.ShapeDtypeStruct((cols, batch), BF16),
            jax.ShapeDtypeStruct(cell_state.shape, F32),
            jax.ShapeDtypeStruct(norm_state.shape, F32),
            jax.ShapeDtypeStruct(max_state.shape, F32),
        ),
        in_specs=[anywhere] * len(operands),
        out_specs=(in_vmem, anywhere, anywhere, in_vmem),
        scratch_shapes=scratch,
        compiler_params=pltpu.CompilerParams(collective_id=0, has_side_effects=True),
        name="decode_step",
    )(*operands)
    return out.T, cell_next, norm_next, max_next


def solution(mesh):
    kv_tp = ("kv", "tp")
    in_specs = (
        P(None, kv_tp),
        P(),
        P("kv", "tp"),
        P("kv", "tp"),
        P("kv", "tp"),
        P("kv", "tp"),
        P("kv", None),
        P(),
        P("kv", "tp", None),
        P("kv", None, None),
        P("kv", None),
        P(),
        P("tp", "kv"),
        P(),
        P("kv", "tp"),
        P("tp", "kv"),
    )
    out_specs = (P(None, kv_tp), P("kv", "tp", None), P("kv", None, None), P("kv", None))
    body = functools.partial(per_device, mesh.shape["kv"], mesh.shape["tp"])
    return jax.shard_map(
        body, mesh=mesh, in_specs=in_specs, out_specs=out_specs, check_vma=False
    )
```

```python
import functools
import math

import jax
import jax.numpy as jnp
from jax import lax
from jax.experimental import pallas as pl
from jax.experimental.pallas import tpu as pltpu
from jax.sharding import PartitionSpec as P

EPSILON = 1e-06
F32 = jnp.float32
BF16 = jnp.bfloat16
MESH = pl.DeviceIdType.MESH


def dot(a, b, ca, cb):
    return lax.dot_general(a, b, (((ca,), (cb,)), ((), ())), preferred_element_type=F32)


def two_parts(total):
    high = total.astype(BF16)
    return jnp.concatenate([high, (total - high.astype(F32)).astype(BF16)], axis=0)


def kernel(
    nkv,
    ntp,
    width,
    tok_ref,
    gmix_ref,
    wq_ref,
    wk_ref,
    wv_ref,
    wo_ref,
    wgt_ref,
    bias_ref,
    cell_ref,
    norm_ref,
    max_ref,
    ggrp_ref,
    wmix_ref,
    gffn_ref,
    wup_ref,
    wdown_ref,
    out_ref,
    cellnext_ref,
    normnext_ref,
    maxnext_ref,
    tok,
    gmix,
    w4,
    wgt,
    bias,
    maxs,
    ggrp,
    wmix,
    gffn,
    wup,
    wdown,
    wqk_other,
    wbig,
    wmixt,
    wupt,
    wdownt,
    cellb,
    ones_tail,
    a_recv,
    b_send,
    b_recv,
    k_send,
    k_recv,
    c_send,
    c_recv,
    d_send,
    d_recv,
    e_send,
    e_recv,
    f_send,
    f_recv,
    g_send,
    g_recv,
    h_send,
    h_recv,
    load_sems,
    send_sems,
    recv_sems,
):
    kv = lax.axis_index("kv")
    tp = lax.axis_index("tp")
    cell, norm = cellnext_ref, normnext_ref
    seqs, rows, hd = cell.shape
    heads = norm.shape[1]
    cols, batch = tok.shape
    block = cols * ntp
    share = g_send.shape[0]
    units = share * nkv
    head = tp * rows // hd
    side = tp % 2
    sibling = tp + 1 - 2 * side
    first = side == 0
    reach = ntp // 8

    loads = []
    for i, (src, dst) in enumerate(
        (
            (tok_ref, tok),
            (wq_ref, w4.at[0]),
            (wk_ref, w4.at[1]),
            (gmix_ref, gmix),
            (wv_ref, w4.at[2]),
            (wo_ref, w4.at[3]),
            (wgt_ref, wgt),
            (bias_ref, bias),
            (cell_ref, cell),
            (norm_ref, norm),
            (max_ref, maxs),
            (ggrp_ref, ggrp),
            (wmix_ref, wmix),
            (gffn_ref, gffn),
            (wup_ref, wup),
            (wdown_ref, wdown),
        )
    ):
        loads.append(pltpu.make_async_copy(src, dst, load_sems.at[i]))
    loads[0].start()

    barrier = pltpu.get_barrier_semaphore()

    def near(i):
        chips = reach - i // 4
        return lax.rem(tp + 2 * chips * (1 - 2 * (i % 2)) + (i // 2) % 2 + ntp - side, ntp)

    def greet_tp(i, _):
        pl.semaphore_signal(barrier, inc=1, device_id=(kv, near(i)), device_id_type=MESH)
        return 0

    def greet_kv(i, _):
        pl.semaphore_signal(barrier, inc=1, device_id=(kv_peer(i), tp), device_id_type=MESH)
        return 0

    def tp_peer(i):
        half = ntp // 2
        return lax.rem(tp + half + (1 - 2 * (i % 2)) * ((i + 1) // 2) + ntp, ntp)

    def kv_peer(i):
        half = nkv // 2
        return lax.rem(kv + half + (1 - 2 * (i % 2)) * ((i + 1) // 2) + nkv, nkv)

    lax.fori_loop(0, 4 * reach, greet_tp, 0)
    lax.fori_loop(0, nkv - 1, greet_kv, 0)
    pl.semaphore_signal(barrier, inc=1, device_id=(kv, sibling), device_id_type=MESH)
    for copy in loads[1:]:
        copy.start()

    def push(phase, src, dst, device):
        pltpu.make_async_remote_copy(
            src_ref=src,
            dst_ref=dst,
            send_sem=send_sems.at[phase],
            recv_sem=recv_sems.at[phase],
            device_id=device,
            device_id_type=MESH,
        ).start()

    def send_tp(phase, src_of, dst):
        def one(i, _):
            peer = tp_peer(i)
            push(phase, src_of(peer), dst.at[tp], (kv, peer))
            return 0

        lax.fori_loop(0, ntp - 1, one, 0)

    def send_kv(phase, src_of, dst):
        def one(i, _):
            peer = kv_peer(i)
            push(phase, src_of(peer), dst.at[kv], (peer, tp))
            return 0

        lax.fori_loop(0, nkv - 1, one, 0)

    def all_of(phase, buf, count):
        part = buf.at[pl.ds(0, count)]
        return pltpu.make_async_remote_copy(
            src_ref=part,
            dst_ref=part,
            send_sem=send_sems.at[phase],
            recv_sem=recv_sems.at[phase],
            device_id=(kv, lax.rem(tp + 1, ntp)),
            device_id_type=MESH,
        )

    def send_near(i, _):
        down = i % 2
        pltpu.make_async_remote_copy(
            src_ref=tok,
            dst_ref=a_recv.at[tp],
            send_sem=send_sems.at[0],
            recv_sem=recv_sems.at[12 + down],
            device_id=(kv, near(i)),
            device_id_type=MESH,
        ).start()
        return 0

    def hand_on(phase, chip, steps, to):
        def one(i, _):
            at = 2 * lax.rem(chip + i + ntp // 2, ntp // 2)
            pair = a_recv.at[pl.ds(at, 2)]
            push(phase, pair, pair, (kv, lax.rem(tp + 2 * to + ntp, ntp)))
            return 0

        lax.fori_loop(0, steps, one, 0)

    loads[0].wait()
    pl.semaphore_wait(barrier, 4 * reach + nkv)
    lax.fori_loop(0, 4 * reach, send_near, 0)
    push(2, tok, a_recv.at[tp], (kv, sibling))
    loads[1].wait()
    loads[2].wait()
    push(3, w4.at[pl.ds(0, 2)], wqk_other, (kv, sibling))
    a_recv[tp] = tok[...]
    chip = tp // 2
    all_of(12, a_recv, 2 * reach).wait_recv()
    if reach > 1:
        hand_on(0, chip - reach + 1, reach - 1, reach)
    all_of(13, a_recv, 2 * reach).wait_recv()
    hand_on(0, chip + 1, reach, -reach)

    for i in range(3, 16):
        loads[i].wait()
    lane_groups = block // 128 if block >= 128 else 1
    lanes = block // lane_groups
    gpieces = []
    for g in range(lane_groups):
        row = gmix[pl.ds(kv * lane_groups + g, 1), :]
        gpieces.append(jnp.transpose(jnp.broadcast_to(row, (128, lanes))))
    gain_col = jnp.concatenate(gpieces, axis=0)
    gain = gain_col[:, :rows]
    wbig[:, 2 * hd : 2 * hd + rows] = (w4[2].astype(F32) * gain).astype(BF16)
    wbig[:, 2 * hd + rows : 2 * hd + 2 * rows] = (w4[3].astype(F32) * gain).astype(BF16)
    wg = jnp.transpose(wgt[...].astype(F32)) * gain_col[:, : 2 * heads]
    tail_at = 2 * hd + 2 * rows
    wbig[:, tail_at:] = jnp.zeros((block, 128), BF16)
    wbig[:, tail_at : tail_at + 2 * heads] = wg.astype(BF16)
    lane_id = lax.broadcasted_iota(jnp.int32, (block, 128), 1)
    ones_tail[...] = jnp.where(lane_id < 2 * heads, 0.0, 1.0).astype(BF16)
    grow = ggrp[pl.ds(tp, 1), :]
    wmixt[...] = (jnp.transpose(wmix[...].astype(F32)) * grow).astype(BF16)
    frow = jnp.concatenate(
        [gffn[pl.ds(kv * lane_groups + g, 1), :] for g in range(lane_groups)], axis=1
    )
    wupt[...] = (jnp.transpose(wup[...].astype(F32)) * frow).astype(BF16)
    wdownt[...] = jnp.transpose(wdown[...].astype(F32)).astype(BF16)
    for s in range(seqs):
        cellb[s] = cell[s].astype(BF16)
    head_of = lax.broadcasted_iota(jnp.int32, (seqs, heads, hd), 1)
    norm_own = jnp.sum(jnp.where(head_of == head, norm[...], 0.0), axis=1)

    pltpu.make_async_remote_copy(
        src_ref=wqk_other,
        dst_ref=wqk_other,
        send_sem=send_sems.at[3],
        recv_sem=recv_sems.at[3],
        device_id=(kv, sibling),
        device_id_type=MESH,
    ).wait_recv()
    for i in range(2):
        mine = w4[i].astype(F32)
        other = wqk_other[i].astype(F32)
        low = jnp.where(first, mine, other)
        high = jnp.where(first, other, mine)
        wbig[:, i * hd : i * hd + rows] = (low * gain).astype(BF16)
        wbig[:, i * hd + rows : (i + 1) * hd] = (high * gain).astype(BF16)

    all_of(2, a_recv, 1).wait_recv()
    all_of(0, a_recv, ntp - 2 - 4 * reach).wait_recv()
    xf = a_recv[...].astype(F32).reshape(block, batch)
    xb = xf.astype(BF16)
    xsq = (xf * xf).astype(BF16)
    part = dot(xb, wbig[...], 0, 0)
    tail = dot(xsq, ones_tail[...], 0, 0)
    b_send[:, :, :tail_at] = part[:, :tail_at].reshape(nkv, seqs, tail_at).astype(BF16)
    b_send[:, :, tail_at:] = (part[:, tail_at:] + tail).reshape(nkv, seqs, 128).astype(BF16)
    send_kv(1, lambda peer: b_send.at[peer], b_recv)
    b_recv[kv] = b_send[kv]
    all_of(1, b_recv, nkv - 1).wait_recv()
    total = b_recv[0].astype(F32)
    for j in range(1, nkv):
        total = total + b_recv[j].astype(F32)
    ends = tail_at + 2 * heads
    scale_in = lax.rsqrt(total[:, ends : ends + 1] / width + EPSILON)
    total = total * scale_in
    qf = total[:, :hd].astype(BF16).astype(F32)
    keys = total[:, hd : 2 * hd].astype(BF16)
    kf = keys.astype(F32) / math.sqrt(hd)
    values = total[:, 2 * hd : 2 * hd + rows]
    gate_out = total[:, 2 * hd + rows : tail_at]
    gate_in = total[:, tail_at : tail_at + heads]
    gate_forget = total[:, tail_at + heads : ends]

    arg = gate_forget + bias[...]
    log_forget = jnp.minimum(arg, 0.0) - jnp.log1p(jnp.exp(-jnp.abs(arg)))
    carried = log_forget + maxs[...]
    max_next = jnp.maximum(carried, gate_in)
    decay = jnp.exp(carried - max_next)
    inflow = jnp.exp(gate_in - max_next)
    maxnext_ref[...] = max_next
    head_lane = lax.broadcasted_iota(jnp.int32, (seqs, heads), 1)
    dec = jnp.sum(jnp.where(head_lane == head, decay, 0.0), axis=1, keepdims=True)
    inf = jnp.sum(jnp.where(head_lane == head, inflow, 0.0), axis=1, keepdims=True)
    gate_sig = jax.nn.sigmoid(gate_out)

    kq = jnp.sum(kf * qf, axis=1, keepdims=True)
    nq = jnp.sum(norm_own * qf, axis=1, keepdims=True)
    denom = jnp.maximum(jnp.abs(dec * nq + inf * kq), 1.0)
    row_id = lax.broadcasted_iota(jnp.int32, (seqs, hd), 0)
    cq = jnp.zeros((seqs, rows), F32)
    for s in range(seqs):
        cq = cq + dot(jnp.where(row_id == s, qf, 0.0).astype(BF16), cellb[s], 1, 1)
    iv = inf * values
    read = gate_sig * ((dec * cq + iv * kq) / denom)

    c_send[...] = read.astype(BF16)
    send_kv(6, lambda peer: c_send, c_recv)
    c_recv[kv] = c_send[...]
    k_send[...] = keys

    def send_keys(i, _):
        half = ntp // 4
        away = half + (1 - 2 * (i % 2)) * ((i + 1) // 2)
        push(4, k_send, k_recv.at[chip], (kv, lax.rem(tp + 2 * away + ntp, ntp)))
        return 0

    lax.fori_loop(0, ntp // 2 - 1, send_keys, 0)
    k_recv[chip] = k_send[...]
    ivt = jnp.transpose(iv)
    for s in range(seqs):
        cell[s] = dec[s : s + 1, :] * cell[s] + ivt[:, s : s + 1] * kf[s : s + 1, :]

    all_of(6, c_recv, nkv - 1).wait_recv()
    rf = c_recv[...].astype(F32).reshape(batch, rows)
    rb = rf.astype(BF16)
    sq = dot(jnp.ones((8, rows), BF16), (rf * rf).astype(BF16), 1, 1)
    d_send[:, cols:, :] = jnp.broadcast_to(two_parts(sq[0:1, :])[None], (ntp, 2, batch))
    mixt = dot(wmixt[...], rb, 1, 1)
    d_send[:, :cols, :] = mixt.reshape(ntp, cols, batch).astype(BF16)
    send_tp(5, lambda peer: d_send.at[peer], d_recv)
    d_recv[tp] = d_send[tp]
    all_of(5, d_recv, ntp - 1).wait_recv()
    both = d_recv[0].astype(F32)
    for j in range(1, ntp):
        both = both + d_recv[j].astype(F32)
    mix_sum = both[:cols]
    sq_sum = both[cols : cols + 1] + both[cols + 1 : cols + 2]
    scale_group = lax.rsqrt(sq_sum / (heads * hd) + EPSILON)
    mixed = (tok[...].astype(F32) + mix_sum * scale_group).astype(BF16)

    e_send[...] = mixed
    send_tp(7, lambda peer: e_send, e_recv)
    e_recv[tp] = e_send[...]
    all_of(7, e_recv, ntp - 1).wait_recv()
    mf = e_recv[...].astype(F32).reshape(block, batch)
    upt = dot(wupt[...], mf.astype(BF16), 1, 0)
    fsq = two_parts(jnp.sum(mf * mf, axis=0, keepdims=True))
    f_send[:, share:, :] = jnp.broadcast_to(fsq[None], (nkv, 2, batch))
    f_send[:, :share, :] = upt.reshape(nkv, share, batch).astype(BF16)
    send_kv(9, lambda peer: f_send.at[peer], f_recv)
    f_recv[kv] = f_send[kv]
    all_of(9, f_recv, nkv - 1).wait_recv()
    both = f_recv[0].astype(F32)
    for j in range(1, nkv):
        both = both + f_recv[j].astype(F32)
    up = both[:share]
    fsq_sum = both[share : share + 1] + both[share + 1 : share + 2]
    scale_ffn = lax.rsqrt(fsq_sum / width + EPSILON)
    hid = jnp.maximum(up * scale_ffn, 0.0)

    g_send[...] = (hid * hid).astype(BF16)
    send_kv(10, lambda peer: g_send, g_recv)
    g_recv[kv] = g_send[...]
    all_of(4, k_recv, ntp // 2 - 1).wait_recv()
    for h in range(heads):
        key = k_recv[h].astype(F32) / math.sqrt(hd)
        norm[:, h, :] = decay[:, h : h + 1] * norm[:, h, :] + inflow[:, h : h + 1] * key

    all_of(10, g_recv, nkv - 1).wait_recv()
    hidden = g_recv[...].reshape(units, batch)
    downt = dot(wdownt[...], hidden, 1, 0)
    h_send[...] = downt.reshape(ntp, cols, batch).astype(BF16)
    send_tp(11, lambda peer: h_send.at[peer], h_recv)
    h_recv[tp] = h_send[tp]

    all_of(0, a_recv, ntp - 2).wait_send()
    all_of(2, a_recv, 1).wait_send()
    pltpu.make_async_remote_copy(
        src_ref=wqk_other,
        dst_ref=wqk_other,
        send_sem=send_sems.at[3],
        recv_sem=recv_sems.at[3],
        device_id=(kv, sibling),
        device_id_type=MESH,
    ).wait_send()
    all_of(1, b_recv, nkv - 1).wait_send()
    all_of(6, c_recv, nkv - 1).wait_send()
    all_of(4, k_recv, ntp // 2 - 1).wait_send()
    all_of(5, d_recv, ntp - 1).wait_send()
    all_of(7, e_recv, ntp - 1).wait_send()
    all_of(9, f_recv, nkv - 1).wait_send()
    all_of(10, g_recv, nkv - 1).wait_send()

    all_of(11, h_recv, ntp - 1).wait_recv()
    down = h_recv[0].astype(F32)
    for j in range(1, ntp):
        down = down + h_recv[j].astype(F32)
    out_ref[...] = (mixed.astype(F32) + down).astype(BF16)
    all_of(11, h_recv, ntp - 1).wait_send()


def write_out(*refs):
    sems = refs[8]
    copies = [pltpu.make_async_copy(refs[i], refs[4 + i], sems.at[i]) for i in range(4)]
    for i in (1, 2, 3, 0):
        copies[i].start()
    for copy in copies:
        copy.wait()


def per_device(nkv, ntp, *args):
    (
        tokens,
        gain_mix,
        w_query,
        w_key,
        w_value,
        w_outgate,
        w_gates,
        forget_bias,
        cell_state,
        norm_state,
        max_state,
        gain_group,
        w_mix,
        gain_ffn,
        w_up,
        w_down,
    ) = args
    batch, cols = tokens.shape
    width = gain_mix.shape[0]
    seqs, rows, hd = cell_state.shape
    heads = forget_bias.shape[0]
    block = w_query.shape[0]
    units = w_up.shape[1]
    share = units // nkv
    lanes = min(block, 128)
    operands = (
        tokens.T,
        gain_mix.reshape(-1, lanes),
        w_query,
        w_key,
        w_value,
        w_outgate,
        w_gates.T,
        forget_bias.reshape(1, heads),
        cell_state,
        norm_state,
        max_state,
        gain_group.reshape(-1, rows),
        w_mix,
        gain_ffn.reshape(-1, lanes),
        w_up,
        w_down,
    )
    wide = 2 * hd + 2 * rows + 128
    vmem = pltpu.VMEM
    scratch = [
        vmem((cols, batch), BF16),
        vmem((width // lanes, lanes), F32),
        vmem((4, block, rows), BF16),
        vmem((2 * heads, block), BF16),
        vmem((1, heads), F32),
        vmem((seqs, heads), F32),
        vmem((heads * hd // rows, rows), F32),
        vmem((rows, block), BF16),
        vmem((width // lanes, lanes), F32),
        vmem((block, units), BF16),
        vmem((units, block), BF16),
        vmem((2, block, rows), BF16),
        vmem((block, wide), BF16),
        vmem((block, rows), BF16),
        vmem((units, block), BF16),
        vmem((block, units), BF16),
        vmem((seqs, rows, hd), BF16),
        vmem((block, 128), BF16),
        vmem((ntp, cols, batch), BF16),
        vmem((nkv, seqs, wide), BF16),
        vmem((nkv, seqs, wide), BF16),
        vmem((seqs, hd), BF16),
        vmem((ntp // 2, seqs, hd), BF16),
        vmem((seqs, rows), BF16),
        vmem((nkv, seqs, rows), BF16),
        vmem((ntp, cols + 2, batch), BF16),
        vmem((ntp, cols + 2, batch), BF16),
        vmem((cols, batch), BF16),
        vmem((ntp, cols, batch), BF16),
        vmem((nkv, share + 2, batch), BF16),
        vmem((nkv, share + 2, batch), BF16),
        vmem((share, batch), BF16),
        vmem((nkv, share, batch), BF16),
        vmem((ntp, cols, batch), BF16),
        vmem((ntp, cols, batch), BF16),
        pltpu.SemaphoreType.DMA((16,)),
        pltpu.SemaphoreType.DMA((14,)),
        pltpu.SemaphoreType.DMA((14,)),
    ]
    anywhere = pl.BlockSpec(memory_space=pl.ANY)
    in_vmem = pl.BlockSpec(memory_space=pltpu.VMEM)
    shapes = (
        ((cols, batch), BF16),
        (cell_state.shape, F32),
        (norm_state.shape, F32),
        (max_state.shape, F32),
    )
    results = pl.pallas_call(
        functools.partial(kernel, nkv, ntp, width),
        out_shape=tuple(pltpu.VMEM(shape, dtype) for shape, dtype in shapes),
        in_specs=[pl.BlockSpec(memory_space=pltpu.HBM)] * len(operands),
        out_specs=(in_vmem,) * 4,
        scratch_shapes=scratch,
        compiler_params=pltpu.CompilerParams(
            collective_id=0, has_side_effects=True, vmem_limit_bytes=24 * 1024 * 1024
        ),
        name="decode_step",
    )(*[pltpu.with_memory_space_constraint(x, pltpu.HBM) for x in operands])
    out, cell_next, norm_next, max_next = pl.pallas_call(
        write_out,
        out_shape=tuple(jax.ShapeDtypeStruct(shape, dtype) for shape, dtype in shapes),
        in_specs=[anywhere] * 4,
        out_specs=(anywhere,) * 4,
        scratch_shapes=[pltpu.SemaphoreType.DMA((4,))],
        compiler_params=pltpu.CompilerParams(vmem_limit_bytes=2 * 1024 * 1024),
        name="write_out",
    )(*results)
    return out.T, cell_next, norm_next, max_next


def solution(mesh):
    kv_tp = ("kv", "tp")
    in_specs = (
        P(None, kv_tp),
        P(),
        P("kv", "tp"),
        P("kv", "tp"),
        P("kv", "tp"),
        P("kv", "tp"),
        P("kv", None),
        P(),
        P("kv", "tp", None),
        P("kv", None, None),
        P("kv", None),
        P(),
        P("tp", "kv"),
        P(),
        P("kv", "tp"),
        P("tp", "kv"),
    )
    out_specs = (P(None, kv_tp), P("kv", "tp", None), P("kv", None, None), P("kv", None))
    body = functools.partial(per_device, mesh.shape["kv"], mesh.shape["tp"])
    return jax.shard_map(
        body, mesh=mesh, in_specs=in_specs, out_specs=out_specs, check_vma=False
    )
```
